32 devices in a mesh: sp: 16 (over z, y, x), tp: 2 (over core).
Axes of the slice: x: 2, y: 2, z: 4, core: 2. Of those that a mesh axis runs over, the one named last changes fastest.
Arguments:
- tokens: bfloat16 [4096, 2048], P('sp', 'tp'), may hold values from -6 to 6
- norm_gain: float32 [2048], replicated, may hold values from 0.1 to 1.9
- query_weight: bfloat16 [2048, 1024], P(None, 'tp'), may hold values from -0.18782524 to 0.18782524
- key_weight: bfloat16 [2048, 1024], P(None, 'tp'), may hold values from -0.18782524 to 0.18782524
- value_weight: bfloat16 [2048, 1024], P(None, 'tp'), may hold values from -0.125 to 0.125
- gate_weight: bfloat16 [2048, 1024], P(None, 'tp'), may hold values from -0.125 to 0.125
- outer_weight: bfloat16 [2048, 1024], P(None, 'tp'), may hold values from -0.125 to 0.125
- inner_weight: bfloat16 [2048, 1024], P(None, 'tp'), may hold values from -0.125 to 0.125
- signal_weight: bfloat16 [2048, 1024], P(None, 'tp'), may hold values from -0.125 to 0.125
- conv_taps: float32 [3, 1024], P(None, 'tp'), may hold values from -3.5 to 3.5
- lambdas: float32 [8], P('tp'), may hold values from 0.3 to 0.8
- head_gain: float32 [1024], P('tp'), may hold values from 0.1 to 1.9
- attn_out_weight: bfloat16 [1024, 2048], P('tp'), may hold values from -0.125 to 0.125
- conv_out_weight: bfloat16 [1024, 2048], P('tp'), may hold values from -0.125 to 0.125
Outputs:
- mixed: bfloat16 [4096, 2048], P(('sp', 'tp'))
- log_totals: float32 [8, 2, 4096], P('tp', None, 'sp')
The draws below stay inside these ranges and needn't reach their ends.
All inputs are finite; a program needn't handle non-finite values.
Results may differ from the reference program's by a relative error of at most 0.014.
Values may be sent and summed in bfloat16 or wider, within the bound.
A program may use at most 128 MiB of HBM per device.

```python
import jax
import jax.numpy as jnp
from jax import lax

D = 2048
HEADS = 8
QK = 64
VD = 128
CONV = 1024
KERNEL = 3
TOKENS = 4096
N_TP = 2


def projection_pair(key):
    columns = HEADS * 2 * QK
    spread = 1.4 * D ** (-0.5)
    query_part = jnp.clip(jax.random.normal(jax.random.fold_in(key, 101), (D, columns), jnp.float32), -6.0, 6.0) * spread
    key_part = jnp.clip(jax.random.normal(jax.random.fold_in(key, 102), (D, columns), jnp.float32), -6.0, 6.0) * spread
    return (query_part, key_part)


def draw_query_weight(key, part):
    return projection_pair(key)[0].astype(jnp.bfloat16)


def draw_key_weight(key, part):
    return projection_pair(key)[1].astype(jnp.bfloat16)


def draw_tokens(key, part):
    base = jnp.clip(jax.random.normal(jax.random.fold_in(key, 201), (TOKENS, D), jnp.float32), -6.0, 6.0)
    return base.astype(jnp.bfloat16)


def steps_of(own_key, extent, cuts, smallest, high):
    def one(axis_at, parts):
        heights = jax.random.uniform(jax.random.fold_in(jax.random.fold_in(own_key, 6), axis_at), (parts,), jnp.float32, smallest / len(cuts), high / len(cuts))
        return jnp.repeat(jnp.exp(heights), extent[axis_at] // parts).reshape((-1,) + (1,) * (len(extent) - axis_at - 1))

    loudness = one(*cuts[0])
    for cut in cuts[1:]:
        loudness = loudness * one(*cut)
    return loudness


def noise(key, shape, scale, reach, split=(), kind=jnp.bfloat16):
    factor_of = steps_of(key, shape, split, -0.22, 0.18) if split else 1.0
    array = jax.random.normal(key, shape, jnp.float32) * scale * factor_of
    return jnp.minimum(jnp.maximum(array, -reach), reach).astype(kind)


def setup_inputs(seed: int = 0) -> dict:
    arg_keys = jax.random.split(jax.random.key(seed), 15)
    tokens = draw_tokens(jax.random.fold_in(arg_keys[14], 71), 0)
    norm_gain = jnp.clip(1.0 + 0.18 * jax.random.normal(arg_keys[1], (D,), jnp.float32), 0.1, 1.9)
    query_weight = draw_query_weight(jax.random.fold_in(arg_keys[14], 71), 0)
    key_weight = draw_key_weight(jax.random.fold_in(arg_keys[14], 71), 0)
    value_weight = noise(arg_keys[4], (D, HEADS * VD), D ** -0.5, 0.125, ((1, 2),))
    gate_weight = noise(arg_keys[5], (D, HEADS * VD), D ** -0.5, 0.125, ((1, 2),))
    outer_weight = noise(arg_keys[6], (D, CONV), D ** -0.5, 0.125, ((1, 2),))
    inner_weight = noise(arg_keys[7], (D, CONV), D ** -0.5, 0.125, ((1, 2),))
    signal_weight = noise(arg_keys[8], (D, CONV), D ** -0.5, 0.125, ((1, 2),))
    conv_taps = noise(arg_keys[9], (KERNEL, CONV), KERNEL ** -0.5, 3.5, ((1, 2),), jnp.float32)
    lambdas = jnp.clip(0.3 + 0.5 * jax.random.uniform(arg_keys[10], (HEADS,), jnp.float32) ** steps_of(arg_keys[10], (HEADS,), ((0, 2),), -0.2, 0.2), 0.3, 0.8)
    head_gain = jnp.clip(1.0 + 0.18 * jax.random.normal(arg_keys[11], (HEADS * VD,), jnp.float32), 0.1, 1.9)
    attn_out_weight = noise(arg_keys[12], (HEADS * VD, D), (HEADS * VD + CONV) ** -0.5, 0.125, ((0, 2),))
    conv_out_weight = noise(arg_keys[13], (CONV, D), (HEADS * VD + CONV) ** -0.5, 0.125, ((0, 2),))
    return dict(tokens=tokens, norm_gain=norm_gain, query_weight=query_weight, key_weight=key_weight, value_weight=value_weight, gate_weight=gate_weight, outer_weight=outer_weight, inner_weight=inner_weight, signal_weight=signal_weight, conv_taps=conv_taps, lambdas=lambdas, head_gain=head_gain, attn_out_weight=attn_out_weight, conv_out_weight=conv_out_weight)


def reference(tokens, norm_gain, query_weight, key_weight, value_weight, gate_weight, outer_weight, inner_weight, signal_weight, conv_taps, lambdas, head_gain, attn_out_weight, conv_out_weight):
    tokens_f = tokens.astype(jnp.float32)
    scale = lax.rsqrt(lax.optimization_barrier(jnp.mean(tokens_f * tokens_f, axis=-1, keepdims=True)) + 1e-06)
    normed_in = (tokens_f * norm_gain).astype(jnp.bfloat16)

    def project(weight):
        return (jnp.dot(normed_in.astype(jnp.float32), weight.astype(jnp.float32), preferred_element_type=jnp.float32) * scale).astype(jnp.bfloat16)
    query = project(query_weight)
    key = project(key_weight)
    value = project(value_weight)
    attn_gate = project(gate_weight)
    outer = project(outer_weight)
    inner = project(inner_weight)
    signal = project(signal_weight)
    query_heads = query.reshape(TOKENS, HEADS, 2, QK)
    key_heads = key.reshape(TOKENS, HEADS, 2, QK).astype(jnp.float32)
    value_heads = value.reshape(TOKENS, HEADS, VD).astype(jnp.float32)
    block_rows = 256 if TOKENS % 256 == 0 else 128
    key_pos = jnp.arange(TOKENS, dtype=jnp.int32)

    def one_block(index):
        query_block = lax.dynamic_slice_in_dim(query_heads, (index * block_rows).astype(jnp.int32), block_rows, 0).astype(jnp.float32)
        query_pos = index * block_rows + jnp.arange(block_rows, dtype=jnp.int32)
        score = jnp.einsum('qhmd,khmd->hmqk', query_block, key_heads) * QK ** (-0.5)
        visible = query_pos[:, None] >= key_pos[None, :]
        score = jnp.where(visible, score, -1e+30)
        top = lax.optimization_barrier(jnp.max(score, axis=-1, keepdims=True))
        weights = jnp.exp(score - top)
        total = lax.optimization_barrier(jnp.sum(weights, axis=-1, keepdims=True))
        summed = jnp.einsum('hmqk,khd->hmqd', weights.astype(jnp.bfloat16).astype(jnp.float32), value_heads)
        mapped = summed / total
        diff = mapped[:, 0] - lambdas[:, None, None] * mapped[:, 1]
        log_total = jnp.log(total[..., 0]) + top[..., 0]
        return (jnp.transpose(diff, (1, 0, 2)), log_total)
    diffs, log_parts = lax.map(one_block, jnp.arange(TOKENS // block_rows, dtype=jnp.int32))
    diff = diffs.reshape(TOKENS, HEADS, VD)
    log_totals = jnp.transpose(log_parts, (1, 2, 0, 3)).reshape(HEADS, 2, TOKENS)
    normed = diff * lax.rsqrt(lax.optimization_barrier(jnp.mean(diff * diff, axis=-1, keepdims=True)) + 1e-05) * head_gain.reshape(HEADS, VD)
    head_out = (normed.reshape(TOKENS, HEADS * VD) * jax.nn.silu(attn_gate.astype(jnp.float32))).astype(jnp.bfloat16)
    inner_sig = (inner.astype(jnp.float32) * signal.astype(jnp.float32)).astype(jnp.bfloat16)
    padded = jnp.pad(inner_sig.astype(jnp.float32), ((KERNEL - 1, 0), (0, 0)))
    convolved = jnp.zeros((TOKENS, CONV), jnp.float32)
    for offset in range(KERNEL):
        convolved = convolved + conv_taps[offset] * padded[offset:offset + TOKENS]
    conv_out = (outer.astype(jnp.float32) * convolved).astype(jnp.bfloat16)
    head_cols = HEADS * VD // N_TP
    conv_cols = CONV // N_TP

    def add_group(accum, group):
        head_part = lax.dynamic_slice_in_dim(head_out, (group * head_cols).astype(jnp.int32), head_cols, 1)
        head_rows = lax.dynamic_slice_in_dim(attn_out_weight, (group * head_cols).astype(jnp.int32), head_cols, 0)
        conv_part = lax.dynamic_slice_in_dim(conv_out, (group * conv_cols).astype(jnp.int32), conv_cols, 1)
        conv_rows = lax.dynamic_slice_in_dim(conv_out_weight, (group * conv_cols).astype(jnp.int32), conv_cols, 0)
        partial_value = jnp.dot(head_part.astype(jnp.float32), head_rows.astype(jnp.float32), preferred_element_type=jnp.float32) + jnp.dot(conv_part.astype(jnp.float32), conv_rows.astype(jnp.float32), preferred_element_type=jnp.float32)
        rounded = lax.optimization_barrier(partial_value.astype(jnp.bfloat16))
        return (accum + rounded.astype(jnp.float32), None)
    accum, _ = lax.scan(add_group, jnp.zeros((TOKENS, D), jnp.float32), jnp.arange(N_TP, dtype=jnp.int32))
    return (accum.astype(jnp.bfloat16), log_totals)
```

```python
import functools
import math

import jax
import jax.numpy as jnp
from jax import lax
from jax.experimental import pallas as pl
from jax.experimental.pallas import tpu as pltpu
from jax.sharding import PartitionSpec as P

MESH = pl.DeviceIdType.MESH


def passed_along(shard, axis, by):
    count = lax.axis_size(axis)
    pairs = [(i, i + by) for i in range(count) if 0 <= i + by < count]
    return lax.ppermute(shard, axis, pairs)


def per_device(
    tokens,
    norm_gain,
    query_weight,
    key_weight,
    value_weight,
    gate_weight,
    outer_weight,
    inner_weight,
    signal_weight,
    conv_taps,
    lambdas,
    head_gain,
    attn_out_weight,
    conv_out_weight,
):
    row_count = tokens.shape[0]
    width = norm_gain.shape[0]
    weights = [
        query_weight,
        key_weight,
        value_weight,
        gate_weight,
        outer_weight,
        inner_weight,
        signal_weight,
    ]
    splits = []
    running = 0
    for weight in weights[:-1]:
        running = running + weight.shape[1]
        splits.append(running)
    joined = jnp.concatenate(weights, axis=1)
    empty = jnp.zeros((row_count, joined.shape[1]), jnp.float32)
    piece = lax.all_gather(tokens, "tp", axis=1, tiled=True)
    summed = empty
    piece_f = piece.astype(jnp.float32)
    normed_piece = (piece.astype(jnp.float32) * norm_gain).astype(jnp.bfloat16)
    raw = jnp.dot(normed_piece, joined, preferred_element_type=jnp.float32)
    squares = jnp.sum(piece_f * piece_f, axis=-1)
    scale = lax.rsqrt(squares / width + 1e-06)
    projected = (raw * scale[:, None]).astype(jnp.bfloat16)
    query, key, value, attn_gate, outer, inner, signal = jnp.split(projected, splits, axis=1)
    head_count = lambdas.shape[0]
    key_size = query_weight.shape[1] // (head_count * 2)
    value_size = value_weight.shape[1] // head_count
    score_scale = key_size ** (-0.5)
    own_index = lax.axis_index("sp")
    local_pos = jnp.arange(row_count, dtype=jnp.int32)
    query_parts = [query]
    position_parts = [own_index * row_count + local_pos]
    query_parts = [
        segment.reshape(segment.shape[0], head_count, 2, key_size) for segment in query_parts
    ]

    def absorb(current, query_rows, row_pos, key_block, value_block, key_pos):
        running_max, summed, accum = current
        score = (
            jnp.einsum("qhmd,khmd->hmqk", query_rows, key_block, preferred_element_type=jnp.float32)
            * score_scale
        )
        visible = row_pos[:, None] >= key_pos[None, :]
        masked = jnp.where(visible, score, -1e30)
        new_max = jnp.maximum(running_max, jnp.max(masked, axis=-1, keepdims=True))
        weights_now = jnp.where(visible, jnp.exp(masked - new_max), 0.0)
        factor = jnp.exp(running_max - new_max)
        summed = summed * factor + jnp.sum(weights_now, axis=-1, keepdims=True)
        accum = accum * factor + jnp.einsum(
            "hmqk,khd->hmqd",
            weights_now.astype(jnp.bfloat16),
            value_block,
            preferred_element_type=jnp.float32,
        )
        return (new_max, summed, accum)

    def fresh(rows):
        return (
            jnp.full((head_count, 2, rows, 1), -1e30, jnp.float32),
            jnp.zeros((head_count, 2, rows, 1), jnp.float32),
            jnp.zeros((head_count, 2, rows, value_size), jnp.float32),
        )

    start_states = tuple((fresh(segment.shape[0]) for segment in query_parts))
    carry = start_states
    key_piece = lax.all_gather(key, "sp", axis=0, tiled=True)
    value_piece = lax.all_gather(value, "sp", axis=0, tiled=True)
    length = key_piece.shape[0]
    block_len = 512
    key_blocks = key_piece.reshape(length // block_len, block_len, head_count, 2, key_size)
    value_blocks = value_piece.reshape(length // block_len, block_len, head_count, value_size)

    def one_block(states, item):
        key_block, value_block, block_id = item
        first_key = block_id * block_len
        key_pos = first_key + jnp.arange(block_len, dtype=jnp.int32)
        updated = []
        for current, query_rows, row_pos in zip(states, query_parts, position_parts):

            def compute(held, query_rows=query_rows, row_pos=row_pos):
                return absorb(held, query_rows, row_pos, key_block, value_block, key_pos)

            def unchanged(held):
                return held

            updated.append(
                lax.cond(first_key <= row_pos[row_pos.shape[0] - 1], compute, unchanged, current)
            )
        return (tuple(updated), None)

    carry, _ = lax.scan(
        one_block,
        carry,
        (key_blocks, value_blocks, jnp.arange(length // block_len, dtype=jnp.int32)),
    )
    states = carry
    running_max = jnp.concatenate([held[0] for held in states], axis=2)
    summed = jnp.concatenate([held[1] for held in states], axis=2)
    accum = jnp.concatenate([held[2] for held in states], axis=2)
    mapped = accum / summed
    diff = mapped[:, 0] - lambdas[:, None, None] * mapped[:, 1]
    log_totals = jnp.log(summed[..., 0]) + running_max[..., 0]
    diff = jnp.transpose(diff, (1, 0, 2))
    normed = (
        diff
        * lax.rsqrt(jnp.mean(diff * diff, axis=-1, keepdims=True) + 1e-05)
        * head_gain.reshape(head_count, value_size)
    )
    normed = normed.reshape(row_count, head_count * value_size)
    head_out = (normed * jax.nn.silu(attn_gate.astype(jnp.float32))).astype(jnp.bfloat16)
    taps = conv_taps.shape[0]
    inner_sig = (inner.astype(jnp.float32) * signal.astype(jnp.float32)).astype(jnp.bfloat16)
    before = passed_along(inner_sig[row_count - (taps - 1) :], "sp", 1)
    extended = jnp.concatenate([before, inner_sig], axis=0).astype(jnp.float32)
    convolved = jnp.zeros((row_count, inner_sig.shape[1]), jnp.float32)
    for position in range(taps):
        convolved = convolved + conv_taps[position] * extended[position : position + row_count]
    conv_out = (outer.astype(jnp.float32) * convolved).astype(jnp.bfloat16)
    mixed = lax.psum_scatter(
        (
            jnp.dot(head_out, attn_out_weight, preferred_element_type=jnp.float32)
            + jnp.dot(conv_out, conv_out_weight, preferred_element_type=jnp.float32)
        ).astype(jnp.bfloat16),
        "tp",
        scatter_dimension=0,
        tiled=True,
    )
    return (mixed, log_totals)


RELAY = 4


def fused_kernel(
    sp_count,
    heads,
    tokens_ref,
    gain_ref,
    wq_hbm,
    wk_hbm,
    wv_hbm,
    wg_hbm,
    wouter_hbm,
    winner_hbm,
    wsignal_hbm,
    taps_ref,
    lambdas_ref,
    head_gain_ref,
    wo_hbm,
    wc_hbm,
    mixed_ref,
    totals_ref,
    other_tokens,
    normed,
    w_vmem,
    wo_vmem,
    wc_vmem,
    kv_send,
    q_send,
    kv_all,
    q_all,
    row_max,
    accum,
    gate,
    outer,
    inner_sig,
    tail_in,
    extended,
    conv_out,
    head_out,
    conv_part,
    o_send,
    o_all,
    lt_send,
    lt_all,
    part_send,
    part_recv,
    w_sem,
    tok_sem,
    tail_sem,
    part_sem,
    stage_s,
    stage_r,
    q_s,
    q_r,
    x_s,
    x_r,
    y_s,
    y_r,
    dx_s,
    dx_r,
    dy_s,
    dy_r,
    o_s,
    o_r,
    lt_s,
    lt_r,
    local_sem,
):
    rows, half = tokens_ref.shape
    width = 2 * half
    local = wq_hbm.shape[1]
    lanes = local // heads
    s = lax.axis_index("sp")
    t = lax.axis_index("tp")
    plane = s // RELAY
    member = lax.rem(s, RELAY)
    right_in_pair = member + 1 - 2 * lax.rem(member, 2)
    across = lax.rem(member + 2, RELAY)
    x_dev = plane * RELAY + right_in_pair
    y_dev = plane * RELAY + across
    following = lax.rem(s + 1, sp_count)
    preceding = lax.rem(s + sp_count - 1, sp_count)

    def at(sp_index, tp_index=None):
        return {"sp": sp_index, "tp": t if tp_index is None else tp_index}

    def remote(src, dst, send_sem, recv_sem, device):
        return pltpu.make_async_remote_copy(
            src_ref=src,
            dst_ref=dst,
            send_sem=send_sem,
            recv_sem=recv_sem,
            device_id=device,
            device_id_type=MESH,
        )

    sources = [wk_hbm, wv_hbm, wq_hbm, winner_hbm, wsignal_hbm, wouter_hbm, wg_hbm]
    weight_copies = [
        pltpu.make_async_copy(ref, w_vmem.at[i], w_sem.at[i]) for i, ref in enumerate(sources)
    ]
    weight_copies.append(pltpu.make_async_copy(wc_hbm, wc_vmem, w_sem.at[len(sources)]))
    weight_copies.append(pltpu.make_async_copy(wo_hbm, wo_vmem, w_sem.at[len(sources) + 1]))
    for copy in weight_copies:
        copy.start()

    barrier = pltpu.get_barrier_semaphore()
    greeted = [at(s, 1 - t), at(x_dev), at(y_dev), at(following), at(preceding)]
    for step in range(1, heads):
        greeted.append(at(lax.rem(plane + step, heads) * RELAY + member))
    for device in greeted:
        pl.semaphore_signal(barrier, inc=1, device_id=device, device_id_type=MESH)
    pl.semaphore_wait(barrier, len(greeted))

    tokens_out = remote(tokens_ref, other_tokens, tok_sem.at[0], tok_sem.at[1], at(s, 1 - t))
    tokens_out.start()

    row_max[...] = jnp.full(row_max.shape, -1e30, jnp.float32)
    accum[...] = jnp.zeros(accum.shape, jnp.float32)

    mine = pl.ds(pl.multiple_of(t * half, half), half)
    theirs = pl.ds(pl.multiple_of((1 - t) * half, half), half)
    own_f = tokens_ref[...].astype(jnp.float32)
    squares = jnp.sum(own_f * own_f, axis=-1, keepdims=True)
    normed[:, mine] = (own_f * gain_ref[:, mine]).astype(jnp.bfloat16)
    tokens_out.wait()
    other_f = other_tokens[...].astype(jnp.float32)
    squares = squares + jnp.sum(other_f * other_f, axis=-1, keepdims=True)
    normed[:, theirs] = (other_f * gain_ref[:, theirs]).astype(jnp.bfloat16)
    scale = lax.rsqrt(squares / width + 1e-06)

    def project(index):
        weight_copies[index].wait()
        raw = jnp.dot(normed[...], w_vmem[index], preferred_element_type=jnp.float32)
        return (raw * scale).astype(jnp.bfloat16)

    for index in range(2):
        projected = project(index)
        for h in range(heads):
            kv_send[h, :, index * lanes : (index + 1) * lanes] = projected[
                :, h * lanes : (h + 1) * lanes
            ]

    started = []

    def launch(copy):
        copy.start()
        started.append(copy)

    def block(plane_index, place):
        return kv_all.at[plane_index * RELAY + place]

    keep = pltpu.make_async_copy(kv_send.at[plane], kv_all.at[s], local_sem.at[0])
    keep.start()
    own_block = kv_send.at[plane]
    launch(remote(own_block, kv_all.at[s], x_s.at[0], x_r.at[plane], at(x_dev)))
    launch(remote(own_block, kv_all.at[s], y_s.at[0], y_r.at[plane], at(y_dev)))
    for step in range(1, heads):
        target = lax.rem(plane + step, heads)
        launch(
            remote(
                kv_send.at[target],
                kv_all.at[s],
                stage_s.at[step],
                stage_r.at[plane],
                at(target * RELAY + member),
            )
        )

    projected = project(2)
    for h in range(heads):
        q_send[h] = projected[:, h * lanes : (h + 1) * lanes]
    keep_q = pltpu.make_async_copy(q_send.at[plane], q_all.at[plane], local_sem.at[1])
    keep_q.start()
    q_copies = []
    for step in range(1, heads):
        target = lax.rem(plane + step, heads)
        q_copy = remote(
            q_send.at[target],
            q_all.at[plane],
            q_s.at[step],
            q_r.at[plane],
            at(target * RELAY + member),
        )
        launch(q_copy)

    inner = project(3).astype(jnp.float32)
    signal = project(4).astype(jnp.float32)
    inner_sig[...] = (inner * signal).astype(jnp.bfloat16)
    tail = tail_in.shape[0]
    launch(
        remote(
            inner_sig.at[pl.ds(rows - tail, tail)],
            tail_in,
            tail_sem.at[0],
            tail_sem.at[1],
            at(following),
        )
    )

    order = [plane] + [k + jnp.where(plane <= k, 1, 0) for k in range(heads - 1)]
    half_rows = rows // 2
    first_half, second_half = pl.ds(0, half_rows), pl.ds(half_rows, half_rows)

    def arrived(dst, recv_sem):
        remote(dst, dst, stage_s.at[0], recv_sem, at(x_dev)).wait_recv()

    def forward_stage(k):
        c = order[k]
        here = block(c, member)
        arrived(here, stage_r.at[c])
        launch(remote(here, here, x_s.at[k], x_r.at[c], at(x_dev)))
        launch(remote(here, here, y_s.at[k], y_r.at[c], at(y_dev)))

    def forward_square(k):
        c = order[k]
        from_x = block(c, right_in_pair)
        arrived(from_x, x_r.at[c])
        piece = from_x.at[first_half]
        launch(remote(piece, piece, dy_s.at[k], dy_r.at[c], at(y_dev)))
        from_y = block(c, across)
        arrived(from_y, y_r.at[c])
        piece = from_y.at[second_half]
        launch(remote(piece, piece, dx_s.at[k], dx_r.at[c], at(x_dev)))

    def finish_plane(k):
        c = order[k]
        diagonal = block(c, RELAY - 1 - member)
        arrived(diagonal.at[first_half], dy_r.at[c])
        arrived(diagonal.at[second_half], dx_r.at[c])

    exponent = (lanes // 2) ** (-0.5) * math.log2(math.e)
    span = RELAY * rows
    lane = lax.broadcasted_iota(jnp.int32, (1, lanes), 1)

    def attend(qi, c, masked):
        held = kv_all[pl.ds(c * RELAY, RELAY)].reshape(span, 2 * lanes)
        keys = held[:, :lanes]
        values = jnp.concatenate(
            [held[:, lanes:], jnp.ones((span, lanes), jnp.bfloat16)], axis=1
        )
        both = q_all[qi]
        for m in range(2):
            of_map = (lane < lanes // 2) if m == 0 else (lane >= lanes // 2)
            query = both * of_map.astype(jnp.float32).astype(jnp.bfloat16)
            score = (
                lax.dot_general(
                    query, keys, (((1,), (1,)), ((), ())), preferred_element_type=jnp.float32
                )
                * exponent
            )
            if masked:
                row = lax.broadcasted_iota(jnp.int32, (rows, span), 0) + member * rows
                col = lax.broadcasted_iota(jnp.int32, (rows, span), 1)
                score = jnp.where(row >= col, score, -1e30)
            before = row_max[2 * qi + m]
            top = jnp.maximum(before, jnp.max(score, axis=-1, keepdims=True))
            weights = jnp.exp2(score - top[:, :1]).astype(jnp.bfloat16)
            factor = jnp.exp2(before - top)[:, :1]
            row_max[2 * qi + m] = top
            accum[2 * qi + m] = accum[2 * qi + m] * factor + jnp.dot(
                weights, values, preferred_element_type=jnp.float32
            )

    def attend_plane(k):
        c = order[k]
        attend(c, c, True)

        for qi in range(1, heads):

            @pl.when(qi > c)
            def _(qi=qi):
                attend(qi, c, False)

    forward_stage(1)
    forward_square(0)
    outer[...] = project(5)
    gate[...] = project(6)

    arrived(tail_in, tail_sem.at[1])
    lead = extended.shape[0] - rows
    before_rows = tail_in[tail - lead :, :].astype(jnp.float32)
    extended[0:lead, :] = jnp.where(s > 0, before_rows, 0.0)
    extended[lead:, :] = inner_sig[...].astype(jnp.float32)
    tap_count = taps_ref.shape[0]
    convolved = jnp.zeros((rows, local), jnp.float32)
    for position in range(tap_count):
        offset = lead - (tap_count - 1) + position
        convolved = convolved + taps_ref[position : position + 1, :] * extended[
            offset : offset + rows, :
        ]
    conv_out[...] = (outer[...].astype(jnp.float32) * convolved).astype(jnp.bfloat16)

    keep.wait()
    keep_q.wait()
    for k in range(1, heads):
        c = order[k]
        arrived(q_all.at[c], q_r.at[c])
    for k in range(heads):
        if k + 2 < heads:
            forward_stage(k + 2)
        if k + 1 < heads:
            forward_square(k + 1)
        finish_plane(k)
        attend_plane(k)
        if k == 0:
            weight_copies[len(sources)].wait()
            conv_part[...] = jnp.dot(
                conv_out[...], wc_vmem[...], preferred_element_type=jnp.float32
            )

    lam = lambdas_ref[plane]
    own_gain = head_gain_ref[:, pl.ds(pl.multiple_of(plane * lanes, lanes), lanes)]
    column = lax.broadcasted_iota(jnp.int32, (rows, lanes), 1)
    keep_o = pltpu.make_async_copy(o_send.at[plane], o_all.at[plane], local_sem.at[2])
    keep_lt = pltpu.make_async_copy(lt_send.at[plane], lt_all.at[plane], local_sem.at[3])
    for step in list(range(1, heads)) + [0]:
        target = lax.rem(plane + step, heads)
        maps = []
        logs = []
        for m in range(2):
            held = accum[2 * target + m]
            total = held[:, lanes:]
            maps.append(held[:, :lanes] / total)
            logs.append(jnp.log(total) + row_max[2 * target + m] * math.log(2.0))
        diff = maps[0] - lam * maps[1]
        mean = jnp.mean(diff * diff, axis=-1, keepdims=True)
        o_send[target] = (diff * lax.rsqrt(mean + 1e-05) * own_gain).astype(jnp.bfloat16)
        turned = jnp.where(column == 0, logs[0], logs[1]).T
        lt_send[target] = turned[: lt_send.shape[1], :]
        if step == 0:
            keep_o.start()
            keep_lt.start()
        else:
            device = at(target * RELAY + member)
            launch(remote(o_send.at[target], o_all.at[plane], o_s.at[step], o_r.at[plane], device))
            launch(
                remote(lt_send.at[target], lt_all.at[plane], lt_s.at[step], lt_r.at[plane], device)
            )
    keep_o.wait()
    keep_lt.wait()
    for step in range(1, heads):
        source = lax.rem(plane + step, heads)
        arrived(o_all.at[source], o_r.at[source])
        arrived(lt_all.at[source], lt_r.at[source])
    for h in range(heads):
        totals_ref[h] = lt_all[h, 0:2, :]
        part = slice(h * lanes, (h + 1) * lanes)
        opened = gate[:, part].astype(jnp.float32)
        opened = opened / (1.0 + jnp.exp(-opened))
        head_out[:, part] = (o_all[h].astype(jnp.float32) * opened).astype(jnp.bfloat16)
    weight_copies[len(sources) + 1].wait()

    def partial_rows(which):
        there = pl.ds(pl.multiple_of(which * half_rows, half_rows), half_rows)
        attn = jnp.dot(head_out[there, :], wo_vmem[...], preferred_element_type=jnp.float32)
        return (attn + conv_part[there, :]).astype(jnp.bfloat16)

    part_send[...] = partial_rows(1 - t)
    exchange = remote(part_send, part_recv, part_sem.at[0], part_sem.at[1], at(s, 1 - t))
    exchange.start()
    own_rows = partial_rows(t).astype(jnp.float32)
    exchange.wait()
    mixed_ref[...] = (own_rows + part_recv[...].astype(jnp.float32)).astype(jnp.bfloat16)
    for copy in started:
        copy.wait_send()


def fused(sp_count, *args):
    tokens, norm_gain, wq = args[0], args[1], args[2]
    lambdas, head_gain = args[10], args[11]
    rows, half = tokens.shape
    heads = lambdas.shape[0]
    local = wq.shape[1]
    lanes = local // heads
    out_width = args[12].shape[1]
    bf16, f32 = jnp.bfloat16, jnp.float32
    vmem = pl.BlockSpec(memory_space=pltpu.VMEM)
    hbm = pl.BlockSpec(memory_space=pl.ANY)
    dma = pltpu.SemaphoreType.DMA
    operands = list(args)
    operands[1] = norm_gain.reshape(1, -1)
    operands[11] = head_gain.reshape(1, -1)
    return pl.pallas_call(
        functools.partial(fused_kernel, sp_count, heads),
        out_shape=(
            jax.ShapeDtypeStruct((rows // 2, out_width), bf16),
            jax.ShapeDtypeStruct((heads, 2, rows), f32),
        ),
        in_specs=[vmem, vmem]
        + [hbm] * 7
        + [vmem, pl.BlockSpec(memory_space=pltpu.SMEM), vmem, hbm, hbm],
        out_specs=(vmem, vmem),
        scratch_shapes=[
            pltpu.VMEM((rows, half), bf16),
            pltpu.VMEM((rows, 2 * half), bf16),
            pltpu.VMEM((7,) + wq.shape, bf16),
            pltpu.VMEM(args[12].shape, bf16),
            pltpu.VMEM(args[13].shape, bf16),
            pltpu.VMEM((heads, rows, 2 * lanes), bf16),
            pltpu.VMEM((heads, rows, lanes), bf16),
            pltpu.VMEM((sp_count, rows, 2 * lanes), bf16),
            pltpu.VMEM((heads, rows, lanes), bf16),
            pltpu.VMEM((2 * heads, rows, lanes), f32),
            pltpu.VMEM((2 * heads, rows, 2 * lanes), f32),
            pltpu.VMEM((rows, local), bf16),
            pltpu.VMEM((rows, local), bf16),
            pltpu.VMEM((rows, local), bf16),
            pltpu.VMEM((16, local), bf16),
            pltpu.VMEM((rows + 8, local), f32),
            pltpu.VMEM((rows, local), bf16),
            pltpu.VMEM((rows, local), bf16),
            pltpu.VMEM((rows, out_width), f32),
            pltpu.VMEM((heads, rows, lanes), bf16),
            pltpu.VMEM((heads, rows, lanes), bf16),
            pltpu.VMEM((heads, 8, rows), f32),
            pltpu.VMEM((heads, 8, rows), f32),
            pltpu.VMEM((rows // 2, out_width), bf16),
            pltpu.VMEM((rows // 2, out_width), bf16),
            dma((9,)),
            dma((2,)),
            dma((2,)),
            dma((2,)),
        ]
        + [dma((heads,)) for _ in range(16)]
        + [dma((4,))],
        compiler_params=pltpu.CompilerParams(
            collective_id=0, has_side_effects=True, vmem_limit_bytes=60 * 1024 * 1024
        ),
    )(*operands)


def fits_square(mesh, heads, rows, key_columns, value_columns):
    return (
        mesh.shape["tp"] == 2
        and mesh.shape["sp"] == heads * RELAY
        and heads > 1
        and rows % 32 == 0
        and key_columns == value_columns == heads * 128
    )


def solution(mesh):
    placed = (
        P("sp", "tp"),
        P(),
        P(None, "tp"),
        P(None, "tp"),
        P(None, "tp"),
        P(None, "tp"),
        P(None, "tp"),
        P(None, "tp"),
        P(None, "tp"),
        P(None, "tp"),
        P("tp"),
        P("tp"),
        P("tp", None),
        P("tp", None),
    )

    def step(*args):
        heads = args[10].shape[0]
        if fits_square(mesh, heads, args[0].shape[0], args[2].shape[1], args[4].shape[1]):
            return fused(mesh.shape["sp"], *args)
        return per_device(*args)

    return jax.shard_map(
        step,
        mesh=mesh,
        in_specs=placed,
        out_specs=(P(("sp", "tp"), None), P("tp", None, "sp")),
        check_vma=False,
    )
```

```python
import functools
import math

import jax
import jax.numpy as jnp
from jax import lax
from jax.experimental import pallas as pl
from jax.experimental.pallas import tpu as pltpu
from jax.sharding import PartitionSpec as P

MESH = pl.DeviceIdType.MESH


def passed_along(shard, axis, by):
    count = lax.axis_size(axis)
    pairs = [(i, i + by) for i in range(count) if 0 <= i + by < count]
    return lax.ppermute(shard, axis, pairs)


def per_device(
    tokens,
    norm_gain,
    query_weight,
    key_weight,
    value_weight,
    gate_weight,
    outer_weight,
    inner_weight,
    signal_weight,
    conv_taps,
    lambdas,
    head_gain,
    attn_out_weight,
    conv_out_weight,
):
    row_count = tokens.shape[0]
    width = norm_gain.shape[0]
    weights = [
        query_weight,
        key_weight,
        value_weight,
        gate_weight,
        outer_weight,
        inner_weight,
        signal_weight,
    ]
    splits = []
    running = 0
    for weight in weights[:-1]:
        running = running + weight.shape[1]
        splits.append(running)
    joined = jnp.concatenate(weights, axis=1)
    empty = jnp.zeros((row_count, joined.shape[1]), jnp.float32)
    piece = lax.all_gather(tokens, "tp", axis=1, tiled=True)
    summed = empty
    piece_f = piece.astype(jnp.float32)
    normed_piece = (piece.astype(jnp.float32) * norm_gain).astype(jnp.bfloat16)
    raw = jnp.dot(normed_piece, joined, preferred_element_type=jnp.float32)
    squares = jnp.sum(piece_f * piece_f, axis=-1)
    scale = lax.rsqrt(squares / width + 1e-06)
    projected = (raw * scale[:, None]).astype(jnp.bfloat16)
    query, key, value, attn_gate, outer, inner, signal = jnp.split(projected, splits, axis=1)
    head_count = lambdas.shape[0]
    key_size = query_weight.shape[1] // (head_count * 2)
    value_size = value_weight.shape[1] // head_count
    score_scale = key_size ** (-0.5)
    own_index = lax.axis_index("sp")
    local_pos = jnp.arange(row_count, dtype=jnp.int32)
    query_parts = [query]
    position_parts = [own_index * row_count + local_pos]
    query_parts = [
        segment.reshape(segment.shape[0], head_count, 2, key_size) for segment in query_parts
    ]

    def absorb(current, query_rows, row_pos, key_block, value_block, key_pos):
        running_max, summed, accum = current
        score = (
            jnp.einsum("qhmd,khmd->hmqk", query_rows, key_block, preferred_element_type=jnp.float32)
            * score_scale
        )
        visible = row_pos[:, None] >= key_pos[None, :]
        masked = jnp.where(visible, score, -1e30)
        new_max = jnp.maximum(running_max, jnp.max(masked, axis=-1, keepdims=True))
        weights_now = jnp.where(visible, jnp.exp(masked - new_max), 0.0)
        factor = jnp.exp(running_max - new_max)
        summed = summed * factor + jnp.sum(weights_now, axis=-1, keepdims=True)
        accum = accum * factor + jnp.einsum(
            "hmqk,khd->hmqd",
            weights_now.astype(jnp.bfloat16),
            value_block,
            preferred_element_type=jnp.float32,
        )
        return (new_max, summed, accum)

    def fresh(rows):
        return (
            jnp.full((head_count, 2, rows, 1), -1e30, jnp.float32),
            jnp.zeros((head_count, 2, rows, 1), jnp.float32),
            jnp.zeros((head_count, 2, rows, value_size), jnp.float32),
        )

    start_states = tuple((fresh(segment.shape[0]) for segment in query_parts))
    carry = start_states
    key_piece = lax.all_gather(key, "sp", axis=0, tiled=True)
    value_piece = lax.all_gather(value, "sp", axis=0, tiled=True)
    length = key_piece.shape[0]
    block_len = 512
    key_blocks = key_piece.reshape(length // block_len, block_len, head_count, 2, key_size)
    value_blocks = value_piece.reshape(length // block_len, block_len, head_count, value_size)

    def one_block(states, item):
        key_block, value_block, block_id = item
        first_key = block_id * block_len
        key_pos = first_key + jnp.arange(block_len, dtype=jnp.int32)
        updated = []
        for current, query_rows, row_pos in zip(states, query_parts, position_parts):

            def compute(held, query_rows=query_rows, row_pos=row_pos):
                return absorb(held, query_rows, row_pos, key_block, value_block, key_pos)

            def unchanged(held):
                return held

            updated.append(
                lax.cond(first_key <= row_pos[row_pos.shape[0] - 1], compute, unchanged, current)
            )
        return (tuple(updated), None)

    carry, _ = lax.scan(
        one_block,
        carry,
        (key_blocks, value_blocks, jnp.arange(length // block_len, dtype=jnp.int32)),
    )
    states = carry
    running_max = jnp.concatenate([held[0] for held in states], axis=2)
    summed = jnp.concatenate([held[1] for held in states], axis=2)
    accum = jnp.concatenate([held[2] for held in states], axis=2)
    mapped = accum / summed
    diff = mapped[:, 0] - lambdas[:, None, None] * mapped[:, 1]
    log_totals = jnp.log(summed[..., 0]) + running_max[..., 0]
    diff = jnp.transpose(diff, (1, 0, 2))
    normed = (
        diff
        * lax.rsqrt(jnp.mean(diff * diff, axis=-1, keepdims=True) + 1e-05)
        * head_gain.reshape(head_count, value_size)
    )
    normed = normed.reshape(row_count, head_count * value_size)
    head_out = (normed * jax.nn.silu(attn_gate.astype(jnp.float32))).astype(jnp.bfloat16)
    taps = conv_taps.shape[0]
    inner_sig = (inner.astype(jnp.float32) * signal.astype(jnp.float32)).astype(jnp.bfloat16)
    before = passed_along(inner_sig[row_count - (taps - 1) :], "sp", 1)
    extended = jnp.concatenate([before, inner_sig], axis=0).astype(jnp.float32)
    convolved = jnp.zeros((row_count, inner_sig.shape[1]), jnp.float32)
    for position in range(taps):
        convolved = convolved + conv_taps[position] * extended[position : position + row_count]
    conv_out = (outer.astype(jnp.float32) * convolved).astype(jnp.bfloat16)
    mixed = lax.psum_scatter(
        (
            jnp.dot(head_out, attn_out_weight, preferred_element_type=jnp.float32)
            + jnp.dot(conv_out, conv_out_weight, preferred_element_type=jnp.float32)
        ).astype(jnp.bfloat16),
        "tp",
        scatter_dimension=0,
        tiled=True,
    )
    return (mixed, log_totals)


RELAY = 4


def fused_kernel(
    sp_count,
    heads,
    tokens_ref,
    gain_ref,
    wq_hbm,
    wk_hbm,
    wv_hbm,
    wg_hbm,
    wouter_hbm,
    winner_hbm,
    wsignal_hbm,
    taps_ref,
    lambdas_ref,
    head_gain_ref,
    wo_hbm,
    wc_hbm,
    mixed_ref,
    totals_ref,
    other_tokens,
    normed,
    w_vmem,
    wo_vmem,
    wc_vmem,
    kv_send,
    q_send,
    kv_all,
    q_all,
    row_max,
    accum,
    gate,
    outer,
    inner_sig,
    tail_in,
    extended,
    conv_out,
    head_out,
    conv_part,
    o_send,
    o_all,
    lt_send,
    lt_all,
    part_send,
    part_recv,
    w_sem,
    tok_sem,
    tail_sem,
    part_sem,
    stage_s,
    stage_r,
    q_s,
    q_r,
    x_s,
    x_r,
    y_s,
    y_r,
    dx_s,
    dx_r,
    dy_s,
    dy_r,
    o_s,
    o_r,
    lt_s,
    lt_r,
    local_sem,
):
    rows, half = tokens_ref.shape
    width = 2 * half
    local = wq_hbm.shape[1]
    lanes = local // heads
    s = lax.axis_index("sp")
    t = lax.axis_index("tp")
    plane = s // RELAY
    member = lax.rem(s, RELAY)
    right_in_pair = member + 1 - 2 * lax.rem(member, 2)
    across = lax.rem(member + 2, RELAY)
    x_dev = plane * RELAY + right_in_pair
    y_dev = plane * RELAY + across
    following = lax.rem(s + 1, sp_count)
    preceding = lax.rem(s + sp_count - 1, sp_count)

    def at(sp_index, tp_index=None):
        return {"sp": sp_index, "tp": t if tp_index is None else tp_index}

    def remote(src, dst, send_sem, recv_sem, device):
        return pltpu.make_async_remote_copy(
            src_ref=src,
            dst_ref=dst,
            send_sem=send_sem,
            recv_sem=recv_sem,
            device_id=device,
            device_id_type=MESH,
        )

    sources = [wk_hbm, wv_hbm, wq_hbm, winner_hbm, wsignal_hbm, wouter_hbm, wg_hbm]
    weight_copies = [
        pltpu.make_async_copy(ref, w_vmem.at[i], w_sem.at[i]) for i, ref in enumerate(sources)
    ]
    weight_copies.append(pltpu.make_async_copy(wc_hbm, wc_vmem, w_sem.at[len(sources)]))
    weight_copies.append(pltpu.make_async_copy(wo_hbm, wo_vmem, w_sem.at[len(sources) + 1]))
    for copy in weight_copies:
        copy.start()

    barrier = pltpu.get_barrier_semaphore()
    greeted = [at(s, 1 - t), at(x_dev), at(y_dev), at(following), at(preceding)]
    for step in range(1, heads):
        greeted.append(at(lax.rem(plane + step, heads) * RELAY + member))
    for device in greeted:
        pl.semaphore_signal(barrier, inc=1, device_id=device, device_id_type=MESH)
    pl.semaphore_wait(barrier, len(greeted))

    tokens_out = remote(tokens_ref, other_tokens, tok_sem.at[0], tok_sem.at[1], at(s, 1 - t))
    tokens_out.start()

    row_max[...] = jnp.full(row_max.shape, -1e30, jnp.float32)
    accum[...] = jnp.zeros(accum.shape, jnp.float32)

    mine = pl.ds(pl.multiple_of(t * half, half), half)
    theirs = pl.ds(pl.multiple_of((1 - t) * half, half), half)
    own_f = tokens_ref[...].astype(jnp.float32)
    squares = jnp.sum(own_f * own_f, axis=-1, keepdims=True)
    normed[:, mine] = (own_f * gain_ref[:, mine]).astype(jnp.bfloat16)
    tokens_out.wait()
    other_f = other_tokens[...].astype(jnp.float32)
    squares = squares + jnp.sum(other_f * other_f, axis=-1, keepdims=True)
    normed[:, theirs] = (other_f * gain_ref[:, theirs]).astype(jnp.bfloat16)
    scale = lax.rsqrt(squares / width + 1e-06)

    def project(index):
        weight_copies[index].wait()
        raw = jnp.dot(normed[...], w_vmem[index], preferred_element_type=jnp.float32)
        return (raw * scale).astype(jnp.bfloat16)

    for index in range(2):
        projected = project(index)
        for h in range(heads):
            kv_send[h, :, index * lanes : (index + 1) * lanes] = projected[
                :, h * lanes : (h + 1) * lanes
            ]

    started = []

    def launch(copy):
        copy.start()
        started.append(copy)

    def block(plane_index, place):
        return kv_all.at[plane_index * RELAY + place]

    keep = pltpu.make_async_copy(kv_send.at[plane], kv_all.at[s], local_sem.at[0])
    keep.start()
    own_block = kv_send.at[plane]
    launch(remote(own_block, kv_all.at[s], x_s.at[0], x_r.at[plane], at(x_dev)))
    launch(remote(own_block, kv_all.at[s], y_s.at[0], y_r.at[plane], at(y_dev)))
    for step in range(1, heads):
        target = lax.rem(plane + step, heads)
        launch(
            remote(
                kv_send.at[target],
                kv_all.at[s],
                stage_s.at[step],
                stage_r.at[plane],
                at(target * RELAY + member),
            )
        )

    projected = project(2)
    for h in range(heads):
        q_send[h] = projected[:, h * lanes : (h + 1) * lanes]
    keep_q = pltpu.make_async_copy(q_send.at[plane], q_all.at[plane], local_sem.at[1])
    keep_q.start()
    q_copies = []
    for step in range(1, heads):
        target = lax.rem(plane + step, heads)
        q_copy = remote(
            q_send.at[target],
            q_all.at[plane],
            q_s.at[step],
            q_r.at[plane],
            at(target * RELAY + member),
        )
        launch(q_copy)

    inner = project(3).astype(jnp.float32)
    signal = project(4).astype(jnp.float32)
    inner_sig[...] = (inner * signal).astype(jnp.bfloat16)
    tail = tail_in.shape[0]
    launch(
        remote(
            inner_sig.at[pl.ds(rows - tail, tail)],
            tail_in,
            tail_sem.at[0],
            tail_sem.at[1],
            at(following),
        )
    )

    order = [plane] + [k + jnp.where(plane <= k, 1, 0) for k in range(heads - 1)]
    half_rows = rows // 2
    first_half, second_half = pl.ds(0, half_rows), pl.ds(half_rows, half_rows)

    def arrived(dst, recv_sem):
        remote(dst, dst, stage_s.at[0], recv_sem, at(x_dev)).wait_recv()

    def forward_stage(k):
        c = order[k]
        here = block(c, member)
        arrived(here, stage_r.at[c])
        launch(remote(here, here, x_s.at[k], x_r.at[c], at(x_dev)))
        launch(remote(here, here, y_s.at[k], y_r.at[c], at(y_dev)))

    def forward_square(k):
        c = order[k]
        from_x = block(c, right_in_pair)
        arrived(from_x, x_r.at[c])
        piece = from_x.at[first_half]
        launch(remote(piece, piece, dy_s.at[k], dy_r.at[c], at(y_dev)))
        from_y = block(c, across)
        arrived(from_y, y_r.at[c])
        piece = from_y.at[second_half]
        launch(remote(piece, piece, dx_s.at[k], dx_r.at[c], at(x_dev)))

    def finish_plane(k):
        c = order[k]
        diagonal = block(c, RELAY - 1 - member)
        arrived(diagonal.at[first_half], dy_r.at[c])
        arrived(diagonal.at[second_half], dx_r.at[c])

    exponent = (lanes // 2) ** (-0.5) * math.log2(math.e)
    span = RELAY * rows
    lane = lax.broadcasted_iota(jnp.int32, (1, lanes), 1)

    def attend(qi, c, masked):
        held = kv_all[pl.ds(c * RELAY, RELAY)].reshape(span, 2 * lanes)
        keys = held[:, :lanes]
        values = jnp.concatenate(
            [held[:, lanes:], jnp.ones((span, lanes), jnp.bfloat16)], axis=1
        )
        both = q_all[qi]
        for m in range(2):
            of_map = (lane < lanes // 2) if m == 0 else (lane >= lanes // 2)
            query = both * of_map.astype(jnp.float32).astype(jnp.bfloat16)
            score = (
                lax.dot_general(
                    query, keys, (((1,), (1,)), ((), ())), preferred_element_type=jnp.float32
                )
                * exponent
            )
            if masked:
                row = lax.broadcasted_iota(jnp.int32, (rows, span), 0) + member * rows
                col = lax.broadcasted_iota(jnp.int32, (rows, span), 1)
                score = jnp.where(row >= col, score, -1e30)
            before = row_max[2 * qi + m]
            top = jnp.maximum(before, jnp.max(score, axis=-1, keepdims=True))
            weights = jnp.exp2(score - top[:, :1]).astype(jnp.bfloat16)
            factor = jnp.exp2(before - top)[:, :1]
            row_max[2 * qi + m] = top
            accum[2 * qi + m] = accum[2 * qi + m] * factor + jnp.dot(
                weights, values, preferred_element_type=jnp.float32
            )

    def attend_same(k):
        attend(order[k], order[k], True)

    def attend_later(k):
        for qi in range(1, heads):

            @pl.when(qi > order[k])
            def _(qi=qi):
                attend(qi, order[k], False)

    outer[...] = project(5)
    gate[...] = project(6)

    def mix_conv():
        arrived(tail_in, tail_sem.at[1])
        lead = extended.shape[0] - rows
        before_rows = tail_in[tail - lead :, :].astype(jnp.float32)
        extended[0:lead, :] = jnp.where(s > 0, before_rows, 0.0)
        extended[lead:, :] = inner_sig[...].astype(jnp.float32)
        tap_count = taps_ref.shape[0]
        convolved = jnp.zeros((rows, local), jnp.float32)
        for position in range(tap_count):
            offset = lead - (tap_count - 1) + position
            convolved = convolved + taps_ref[position : position + 1, :] * extended[
                offset : offset + rows, :
            ]
        conv_out[...] = (outer[...].astype(jnp.float32) * convolved).astype(jnp.bfloat16)
        weight_copies[len(sources)].wait()
        conv_part[...] = jnp.dot(conv_out[...], wc_vmem[...], preferred_element_type=jnp.float32)

    lam = lambdas_ref[plane]
    own_gain = head_gain_ref[:, pl.ds(pl.multiple_of(plane * lanes, lanes), lanes)]
    column = lax.broadcasted_iota(jnp.int32, (rows, lanes), 1)
    keep_o = pltpu.make_async_copy(o_send.at[plane], o_all.at[plane], local_sem.at[2])
    keep_lt = pltpu.make_async_copy(lt_send.at[plane], lt_all.at[plane], local_sem.at[3])

    def returns(target):
        device = at(target * RELAY + member)
        return (
            remote(o_send.at[target], o_all.at[plane], o_s.at[target], o_r.at[plane], device),
            remote(lt_send.at[target], lt_all.at[plane], lt_s.at[target], lt_r.at[plane], device),
        )

    def give_back(target):
        maps = []
        logs = []
        for m in range(2):
            held = accum[2 * target + m]
            total = held[:, lanes:]
            maps.append(held[:, :lanes] / total)
            logs.append(jnp.log(total) + row_max[2 * target + m] * math.log(2.0))
        diff = maps[0] - lam * maps[1]
        mean = jnp.mean(diff * diff, axis=-1, keepdims=True)
        o_send[target] = (diff * lax.rsqrt(mean + 1e-05) * own_gain).astype(jnp.bfloat16)
        turned = jnp.where(column == 0, logs[0], logs[1]).T
        lt_send[target] = turned[: lt_send.shape[1], :]

        @pl.when(plane == target)
        def _():
            keep_o.start()
            keep_lt.start()

        @pl.when(plane != target)
        def _():
            for copy in returns(target):
                copy.start()

    if heads > 1:
        forward_stage(1)
    forward_square(0)
    keep.wait()
    keep_q.wait()
    finish_plane(0)
    attend_same(0)
    for k in range(1, heads):
        if k + 1 < heads:
            forward_stage(k + 1)
        forward_square(k)
    for k in range(1, heads):
        c = order[k]
        arrived(q_all.at[c], q_r.at[c])
    attend_later(0)
    for k in range(1, heads):
        finish_plane(k)
        attend_same(k)
        attend_later(k)
        give_back(k - 1)
        if k == 1:
            mix_conv()
    give_back(heads - 1)
    keep_o.wait()
    keep_lt.wait()
    for step in range(1, heads):
        source = lax.rem(plane + step, heads)
        arrived(o_all.at[source], o_r.at[source])
        arrived(lt_all.at[source], lt_r.at[source])
    for h in range(heads):
        totals_ref[h] = lt_all[h, 0:2, :]
        part = slice(h * lanes, (h + 1) * lanes)
        opened = gate[:, part].astype(jnp.float32)
        opened = opened / (1.0 + jnp.exp(-opened))
        head_out[:, part] = (o_all[h].astype(jnp.float32) * opened).astype(jnp.bfloat16)
    weight_copies[len(sources) + 1].wait()

    def partial_rows(which):
        there = pl.ds(pl.multiple_of(which * half_rows, half_rows), half_rows)
        attn = jnp.dot(head_out[there, :], wo_vmem[...], preferred_element_type=jnp.float32)
        return (attn + conv_part[there, :]).astype(jnp.bfloat16)

    part_send[...] = partial_rows(1 - t)
    exchange = remote(part_send, part_recv, part_sem.at[0], part_sem.at[1], at(s, 1 - t))
    exchange.start()
    own_rows = partial_rows(t).astype(jnp.float32)
    exchange.wait()
    mixed_ref[...] = (own_rows + part_recv[...].astype(jnp.float32)).astype(jnp.bfloat16)
    for copy in started:
        copy.wait_send()
    for target in range(heads):

        @pl.when(plane != target)
        def _(target=target):
            for copy in returns(target):
                copy.wait_send()


def fused(sp_count, *args):
    tokens, norm_gain, wq = args[0], args[1], args[2]
    lambdas, head_gain = args[10], args[11]
    rows, half = tokens.shape
    heads = lambdas.shape[0]
    local = wq.shape[1]
    lanes = local // heads
    out_width = args[12].shape[1]
    bf16, f32 = jnp.bfloat16, jnp.float32
    vmem = pl.BlockSpec(memory_space=pltpu.VMEM)
    hbm = pl.BlockSpec(memory_space=pl.ANY)
    dma = pltpu.SemaphoreType.DMA
    operands = list(args)
    operands[1] = norm_gain.reshape(1, -1)
    operands[11] = head_gain.reshape(1, -1)
    return pl.pallas_call(
        functools.partial(fused_kernel, sp_count, heads),
        out_shape=(
            jax.ShapeDtypeStruct((rows // 2, out_width), bf16),
            jax.ShapeDtypeStruct((heads, 2, rows), f32),
        ),
        in_specs=[vmem, vmem]
        + [hbm] * 7
        + [vmem, pl.BlockSpec(memory_space=pltpu.SMEM), vmem, hbm, hbm],
        out_specs=(vmem, vmem),
        scratch_shapes=[
            pltpu.VMEM((rows, half), bf16),
            pltpu.VMEM((rows, 2 * half), bf16),
            pltpu.VMEM((7,) + wq.shape, bf16),
            pltpu.VMEM(args[12].shape, bf16),
            pltpu.VMEM(args[13].shape, bf16),
            pltpu.VMEM((heads, rows, 2 * lanes), bf16),
            pltpu.VMEM((heads, rows, lanes), bf16),
            pltpu.VMEM((sp_count, rows, 2 * lanes), bf16),
            pltpu.VMEM((heads, rows, lanes), bf16),
            pltpu.VMEM((2 * heads, rows, lanes), f32),
            pltpu.VMEM((2 * heads, rows, 2 * lanes), f32),
            pltpu.VMEM((rows, local), bf16),
            pltpu.VMEM((rows, local), bf16),
            pltpu.VMEM((rows, local), bf16),
            pltpu.VMEM((16, local), bf16),
            pltpu.VMEM((rows + 8, local), f32),
            pltpu.VMEM((rows, local), bf16),
            pltpu.VMEM((rows, local), bf16),
            pltpu.VMEM((rows, out_width), f32),
            pltpu.VMEM((heads, rows, lanes), bf16),
            pltpu.VMEM((heads, rows, lanes), bf16),
            pltpu.VMEM((heads, 8, rows), f32),
            pltpu.VMEM((heads, 8, rows), f32),
            pltpu.VMEM((rows // 2, out_width), bf16),
            pltpu.VMEM((rows // 2, out_width), bf16),
            dma((9,)),
            dma((2,)),
            dma((2,)),
            dma((2,)),
        ]
        + [dma((heads,)) for _ in range(16)]
        + [dma((4,))],
        compiler_params=pltpu.CompilerParams(
            collective_id=0, has_side_effects=True, vmem_limit_bytes=60 * 1024 * 1024
        ),
    )(*operands)


def fits_square(mesh, heads, rows, key_columns, value_columns):
    return (
        mesh.shape["tp"] == 2
        and mesh.shape["sp"] == heads * RELAY
        and heads > 1
        and rows % 32 == 0
        and key_columns == value_columns == heads * 128
    )


def solution(mesh):
    placed = (
        P("sp", "tp"),
        P(),
        P(None, "tp"),
        P(None, "tp"),
        P(None, "tp"),
        P(None, "tp"),
        P(None, "tp"),
        P(None, "tp"),
        P(None, "tp"),
        P(None, "tp"),
        P("tp"),
        P("tp"),
        P("tp", None),
        P("tp", None),
    )

    def step(*args):
        heads = args[10].shape[0]
        if fits_square(mesh, heads, args[0].shape[0], args[2].shape[1], args[4].shape[1]):
            return fused(mesh.shape["sp"], *args)
        return per_device(*args)

    return jax.shard_map(
        step,
        mesh=mesh,
        in_specs=placed,
        out_specs=(P(("sp", "tp"), None), P("tp", None, "sp")),
        check_vma=False,
    )
```
